32 devices in a mesh: sp: 8 (over z, y), tp: 4 (over x, core).
Axes of the slice: x: 2, y: 2, z: 4, core: 2. Of those that a mesh axis runs over, the one named last changes fastest.
Arguments:
- skip_stream: bfloat16 [2048, 2048], P('sp', 'tp'), may hold values from -20 to 20
- narrow_lookup_matrix: bfloat16 [2048, 256], P('sp', 'tp'), may hold values from -6 to 6
- narrow_probe_matrix: bfloat16 [2048, 256], P('sp', 'tp'), may hold values from -6 to 6
- narrow_retention_logits: bfloat16 [2048, 256], P('sp', 'tp'), may hold values from -6 to 16
- broad_lookup_matrix: bfloat16 [2048, 512], P('sp', 'tp'), may hold values from -6 to 6
- broad_probe_matrix: bfloat16 [2048, 512], P('sp', 'tp'), may hold values from -6 to 6
- broad_retention_logits: bfloat16 [2048, 512], P('sp', 'tp'), may hold values from -6 to 16
- content_vectors: bfloat16 [2048, 4, 2, 128], P('sp', 'tp'), may hold values from -6 to 6
- extra_log_retention: float32 [2048, 2, 4], P('sp', None, 'tp'), may hold values from -0.7 to 0
- per_branch_scaling: bfloat16 [4, 2, 128], P('tp'), may hold values from 0.099609375 to 1.8984375
- final_projection_matrix: bfloat16 [1024, 2048], P(None, 'tp'), may hold values from -0.1875 to 0.1875
- channel_blend_scaling: bfloat16 [2048], replicated, may hold values from 0.099609375 to 1.8984375
- switch_expansion_matrix: bfloat16 [2048, 5632], P('sp', 'tp'), may hold values from -0.125 to 0.125
- content_expansion_matrix: bfloat16 [2048, 5632], P('sp', 'tp'), may hold values from -0.125 to 0.125
- convolution_kernel: bfloat16 [3, 2, 5632], P(None, None, 'tp'), may hold values from -3.5 to 3.5
- contraction_matrix: bfloat16 [5632, 2048], P('tp', 'sp'), may hold values from -0.078125 to 0.078125
Outputs:
- mixed: bfloat16 [2048, 2048], P('sp', 'tp')
The draws below stay inside these ranges and needn't reach their ends.
All inputs are finite; a program needn't handle non-finite values.
Results may differ from the reference program's by a relative error of at most 0.011.
Values may be sent and summed in bfloat16 or wider, within the bound.
A program may use at most 64 MiB of HBM per device.

```python
import jax
import jax.numpy as jnp
from jax import lax

D = 2048
FF = 5632
GROUP_HEADS = 4
NARROW_PROBE_DIM = 64
BROAD_PROBE_DIM = 128
DV = 128
BLOCK = 64
TOK_DEV = 256
TOKENS = 2048
N_TP = 4


def decay_draw(key, model_width):
    subkeys = jax.random.split(key, 5)
    slow_share = 0.5
    slow = jax.random.uniform(subkeys[0], (GROUP_HEADS,)) < slow_share
    slow_rate = jnp.log(10.0) / TOKENS * jax.random.uniform(subkeys[1], (GROUP_HEADS,), minval=0.05, maxval=0.2)
    fast_rate = jax.random.uniform(subkeys[2], (GROUP_HEADS,), minval=0.01, maxval=0.033)
    rate = jnp.where(slow, slow_rate, fast_rate)
    factor = jnp.exp(jax.random.uniform(subkeys[3], (TOKENS // TOK_DEV,), minval=-0.7, maxval=0.7))
    factor = jnp.repeat(factor, TOK_DEV)
    noise = jnp.exp(0.5 * jnp.clip(jax.random.normal(subkeys[4], (TOKENS, GROUP_HEADS, model_width)), -3.0, 3.0))
    strength = rate[None, :, None] * factor[:, None, None] * noise
    preact = -jnp.log(jnp.expm1(16.0 * strength))
    return preact.reshape(TOKENS, GROUP_HEADS * model_width).astype(jnp.bfloat16)


def draw_narrow_retention_logits(key, part):
    return decay_draw(jax.random.fold_in(key, 11), NARROW_PROBE_DIM)


def draw_broad_retention_logits(key, part):
    return decay_draw(jax.random.fold_in(key, 13), BROAD_PROBE_DIM)


def draw_extra_log_retention(key, part):
    subkeys = jax.random.split(jax.random.fold_in(key, 31), 2)
    spots = jax.random.randint(subkeys[0], (4,), 0, TOKENS)
    places = jnp.arange(TOKENS)
    struck = jnp.any(places[:, None] == spots[None, :], axis=1)
    losses = jnp.log(jax.random.uniform(subkeys[1], (TOKENS, 2, GROUP_HEADS), minval=0.5, maxval=0.8))
    return jnp.where(struck[:, None, None], losses, 0.0).astype(jnp.float32)


def draw_skip_stream(key, part):
    subkey = jax.random.fold_in(key, 47)
    column = jnp.arange(D, dtype=jnp.float32) / D
    entries = jnp.clip(jax.random.normal(subkey, (TOKENS, D)), -6.0, 6.0)
    ramp = jnp.exp(jnp.log(3.0) * column)
    return (entries * ramp[None, :]).astype(jnp.bfloat16)


def block_scale(own_key, extent, pieces, smallest, largest):
    level, own = 1.0, jax.random.fold_in(own_key, 6)
    for axis_at, shards_of in pieces:
        draws = jnp.exp(jax.random.uniform(jax.random.fold_in(own, axis_at), (shards_of,), jnp.float32, smallest / len(pieces), largest / len(pieces)))
        level = level * jnp.repeat(draws, extent[axis_at] // shards_of).reshape([-1 if axis == axis_at else 1 for axis in range(len(extent))])
    return level


def scatter_about(rng, extent, spread, reach, pieces=(), kind=jnp.bfloat16):
    values = spread * jax.random.normal(rng, extent, jnp.float32)
    if pieces:
        values = values * block_scale(rng, extent, pieces, -0.22, 0.18)
    return jnp.clip(values, -reach, reach).astype(kind)


def setup_inputs(seed: int = 0) -> dict:
    splits = jax.random.split(jax.random.key(seed), 17)
    return {
        "skip_stream": draw_skip_stream(jax.random.fold_in(splits[16], 71), 0),
        "narrow_lookup_matrix": scatter_about(splits[1], (TOKENS, GROUP_HEADS * NARROW_PROBE_DIM), 1.0, 6.0, ((0, 8), (1, 4))),
        "narrow_probe_matrix": scatter_about(splits[2], (TOKENS, GROUP_HEADS * NARROW_PROBE_DIM), 1.0, 6.0, ((0, 8), (1, 4))),
        "narrow_retention_logits": draw_narrow_retention_logits(jax.random.fold_in(splits[16], 71), 0),
        "broad_lookup_matrix": scatter_about(splits[4], (TOKENS, GROUP_HEADS * BROAD_PROBE_DIM), 1.0, 6.0, ((0, 8), (1, 4))),
        "broad_probe_matrix": scatter_about(splits[5], (TOKENS, GROUP_HEADS * BROAD_PROBE_DIM), 1.0, 6.0, ((0, 8), (1, 4))),
        "broad_retention_logits": draw_broad_retention_logits(jax.random.fold_in(splits[16], 71), 0),
        "content_vectors": scatter_about(splits[7], (TOKENS, GROUP_HEADS, 2, DV), 1.0, 6.0, ((0, 8), (1, 4))),
        "extra_log_retention": draw_extra_log_retention(jax.random.fold_in(splits[16], 71), 0),
        "per_branch_scaling": jnp.clip(1.0 + 0.18 * jax.random.normal(splits[9], (GROUP_HEADS, 2, DV), jnp.float32), 0.099609375, 1.8984375).astype(jnp.bfloat16),
        "final_projection_matrix": scatter_about(splits[10], (2 * GROUP_HEADS * DV, D), (2 * GROUP_HEADS * DV) ** -0.5, 0.1875, ((1, 4),)),
        "channel_blend_scaling": jnp.clip(1.0 + 0.18 * jax.random.normal(splits[11], (D,), jnp.float32), 0.099609375, 1.8984375).astype(jnp.bfloat16),
        "switch_expansion_matrix": scatter_about(splits[12], (D, FF), D ** -0.5, 0.125, ((0, 8), (1, 4))),
        "content_expansion_matrix": scatter_about(splits[13], (D, FF), D ** -0.5, 0.125, ((0, 8), (1, 4))),
        "convolution_kernel": scatter_about(splits[14], (3, 2, FF), 3 ** -0.5, 3.5, ((2, 4),)),
        "contraction_matrix": scatter_about(splits[15], (FF, D), FF ** -0.5, 0.078125, ((0, 4), (1, 8))),
    }


EPSILON = 1e-06
SOFTENING = 16.0
HIGHEST = lax.Precision.HIGHEST

def blocked(array):
    return array.reshape(array.shape[0] // BLOCK, BLOCK, array.shape[1], array.shape[2]).transpose(0, 2, 1, 3)

def gla_group(query_rows, input_keys, values_in, log_decay):
    query_blocks = blocked(query_rows)
    key_blocks = blocked(input_keys)
    value_blocks = blocked(values_in)
    inner = jnp.cumsum(blocked(log_decay), axis=2)
    last = inner[:, :, -1:, :]
    middle = inner[:, :, BLOCK // 2 - 1:BLOCK // 2, :]
    scores = jnp.einsum('nhid,nhjd->nhij', query_blocks * jnp.exp(inner - middle), key_blocks * jnp.exp(middle - inner), precision=HIGHEST)
    lower = jnp.tril(jnp.ones((BLOCK, BLOCK), dtype=bool))
    local_out = jnp.einsum('nhij,nhjv->nhiv', jnp.where(lower, scores, 0.0), value_blocks, precision=HIGHEST)
    query_carry = query_blocks * jnp.exp(inner)
    key_carry = key_blocks * jnp.exp(last - inner)
    fade = jnp.exp(last[:, :, 0, :])

    def advance(state, inputs):
        query_part, key_part, value_part, fade_part = inputs
        output = jnp.einsum('hid,hdv->hiv', query_part, state, precision=HIGHEST)
        state = fade_part[..., None] * state + jnp.einsum('hjd,hjv->hdv', key_part, value_part, precision=HIGHEST)
        return (state, output)
    start = jnp.zeros((query_blocks.shape[1], query_blocks.shape[3], value_blocks.shape[3]), jnp.float32)
    _, carried = lax.scan(advance, start, (query_carry, key_carry, value_blocks, fade))
    total = local_out + carried
    return total.transpose(0, 2, 1, 3).reshape(query_rows.shape[0], total.shape[1], total.shape[3])

def head_norm(output, gain):
    scale = lax.rsqrt(lax.optimization_barrier(jnp.mean(output * output, axis=-1, keepdims=True)) + EPSILON)
    return output * scale * gain.astype(jnp.float32)

def build_arguments(query_rows, input_keys, forget_gates, spike_column, model_width):
    item_count = query_rows.shape[0]
    query_data = query_rows.astype(jnp.float32).reshape(item_count, GROUP_HEADS, model_width) * model_width ** (-0.5)
    key_data = input_keys.astype(jnp.float32).reshape(item_count, GROUP_HEADS, model_width)
    decay_factor = jax.nn.log_sigmoid(forget_gates.astype(jnp.float32).reshape(item_count, GROUP_HEADS, model_width)) / SOFTENING + spike_column[:, :, None]
    return (query_data, key_data, decay_factor)

def reference(skip_stream, narrow_lookup_matrix, narrow_probe_matrix, narrow_retention_logits, broad_lookup_matrix, broad_probe_matrix, broad_retention_logits, content_vectors, extra_log_retention, per_branch_scaling, final_projection_matrix, channel_blend_scaling, switch_expansion_matrix, content_expansion_matrix, convolution_kernel, contraction_matrix):
    item_count = skip_stream.shape[0]
    value_data = content_vectors.astype(jnp.float32)
    narrow_lookup_vector, narrow_probe_vector, narrow_probe_dim = build_arguments(narrow_lookup_matrix, narrow_probe_matrix, narrow_retention_logits, extra_log_retention[:, 0], NARROW_PROBE_DIM)
    broad_lookup_vector, broad_probe_vector, broad_probe_dim = build_arguments(broad_lookup_matrix, broad_probe_matrix, broad_retention_logits, extra_log_retention[:, 1], BROAD_PROBE_DIM)
    out_small = gla_group(narrow_lookup_vector, narrow_probe_vector, value_data[:, :, 0], narrow_probe_dim)
    out_large = gla_group(broad_lookup_vector, broad_probe_vector, value_data[:, :, 1], broad_probe_dim)
    stacked = jnp.stack([head_norm(out_small, per_branch_scaling[:, 0]), head_norm(out_large, per_branch_scaling[:, 1])], axis=2)
    heads_in = stacked.reshape(item_count, 2 * GROUP_HEADS * DV).astype(jnp.bfloat16)
    resid = (skip_stream.astype(jnp.float32) + jnp.dot(heads_in, final_projection_matrix, preferred_element_type=jnp.float32)).astype(jnp.bfloat16)
    resid_data = resid.astype(jnp.float32)
    scale = lax.rsqrt(lax.optimization_barrier(jnp.mean(resid_data * resid_data, axis=1, keepdims=True)) + EPSILON)
    normed = (resid_data * scale * channel_blend_scaling.astype(jnp.float32)).astype(jnp.bfloat16)
    padded = jnp.concatenate([jnp.zeros((2, normed.shape[1]), jnp.bfloat16), normed], axis=0)
    taps = convolution_kernel.astype(jnp.float32)
    group_width = FF // N_TP

    def convolve(upward, tap_rows):
        return tap_rows[0] * upward[:-2] + tap_rows[1] * upward[1:-1] + tap_rows[2] * upward[2:]

    def mixer_block(index):
        start = (index * TOK_DEV).astype(jnp.int32)
        window = lax.dynamic_slice_in_dim(padded, start, TOK_DEV + 2, 0)
        up_gate = lax.optimization_barrier(jnp.dot(window, switch_expansion_matrix, preferred_element_type=jnp.float32).astype(jnp.bfloat16)).astype(jnp.float32)
        up_value = lax.optimization_barrier(jnp.dot(window, content_expansion_matrix, preferred_element_type=jnp.float32).astype(jnp.bfloat16)).astype(jnp.float32)
        conv_gate = convolve(up_gate, taps[:, 1])
        conv_value = convolve(up_value, taps[:, 0])
        hidden = (jax.nn.silu(conv_gate) * conv_value).astype(jnp.bfloat16)
        summed = jnp.zeros((TOK_DEV, contraction_matrix.shape[1]), jnp.float32)
        for group in range(N_TP):
            partial_product = jnp.dot(hidden[:, group * group_width:(group + 1) * group_width], contraction_matrix[group * group_width:(group + 1) * group_width], preferred_element_type=jnp.float32)
            summed = summed + lax.optimization_barrier(partial_product.astype(jnp.bfloat16)).astype(jnp.float32)
        return summed
    downs = lax.map(mixer_block, jnp.arange(item_count // TOK_DEV, dtype=jnp.int32))
    down = downs.reshape(item_count, contraction_matrix.shape[1])
    return (resid_data + down).astype(jnp.bfloat16)
```

```python
import functools

import jax
import jax.numpy as jnp
from jax import lax
from jax.experimental import pallas as pl
from jax.experimental.pallas import tpu as pltpu
from jax.sharding import PartitionSpec as P

BLOCK = 64
HALO = 16
LANES = 128
GROUP = 4
EPSILON = 1e-06
SOFTENING = 16.0
HIGHEST = lax.Precision.HIGHEST
F32 = jnp.float32
BF16 = jnp.bfloat16
NT = (((1,), (1,)), ((), ()))
TN = (((0,), (0,)), ((), ()))


def exact(a, b, dims):
    return lax.dot_general(a, b, dims, precision=HIGHEST, preferred_element_type=F32)


def local_attention(
    q_refs, k_refs, g_refs, v_ref, extra_ref, out_ref, meets_ref, st_ref
):
    tok, units, dv = v_ref.shape
    key = q_refs[1].shape[1]
    dim = q_refs[0].shape[0]

    def join(refs, scale):
        first = jnp.transpose(refs[0][...].astype(F32))
        second = refs[1][...].astype(F32)
        if scale:
            first = first * dim ** (-0.5)
            second = second * key ** (-0.5)
        if dim < key:
            first = jnp.concatenate([first, jnp.zeros((tok, key - dim), F32)], axis=1)
        return jnp.concatenate([first, second], axis=1)

    gate = join(g_refs, False)
    query_all = join(q_refs, True)
    keys_all = join(k_refs, False)
    soft = jnp.minimum(gate, 0.0) - jnp.log1p(jnp.exp(-jnp.abs(gate)))
    extra = jnp.transpose(
        jnp.concatenate([extra_ref[u] for u in range(units)] + [jnp.zeros((8 - units, tok), F32)], axis=0)
    )
    decay = jnp.concatenate(
        [
            soft[:, u * key : (u + 1) * key] * (1.0 / SOFTENING) + extra[:, u : u + 1]
            for u in range(units)
        ],
        axis=1,
    )
    values_all = v_ref[...].astype(F32)
    row = lax.broadcasted_iota(jnp.int32, (BLOCK, BLOCK), 0)
    col = lax.broadcasted_iota(jnp.int32, (BLOCK, BLOCK), 1)
    lower = row >= col
    tri = jnp.where(lower, 1.0, 0.0)
    plain = (((1,), (0,)), ((), ()))
    before = jnp.zeros((1, units * key), F32)
    state = [jnp.zeros((dv, key), F32) for _ in range(units)]
    for n in range(tok // BLOCK):
        rows = slice(n * BLOCK, (n + 1) * BLOCK)
        inner = exact(tri, decay[rows], plain)
        last = inner[BLOCK - 1 : BLOCK]
        middle = inner[BLOCK // 2 - 1 : BLOCK // 2]
        query = query_all[rows]
        keys = keys_all[rows]
        query_mid = query * jnp.exp(inner - middle)
        key_mid = keys * jnp.exp(middle - inner)
        query_carry = query * jnp.exp(inner)
        key_carry = keys * jnp.exp(last - inner)
        meets_ref[rows] = query_carry * jnp.exp(before)
        gone = jnp.exp(last)
        for u in range(units):
            at = slice(u * key, (u + 1) * key)
            vu = values_all[rows, u, :]
            scores = exact(query_mid[:, at], key_mid[:, at], NT)
            out = exact(jnp.where(lower, scores, 0.0), vu, plain)
            if n:
                out = out + exact(query_carry[:, at], state[u], NT)
            out_ref[rows, u * dv : (u + 1) * dv] = out
            state[u] = gone[:, at] * state[u] + exact(vu, key_carry[:, at], TN)
        before = before + last
    fade = jnp.exp(before)
    upper = dv // 2
    st_ref[:dv] = state[1].astype(BF16)
    st_ref[dv : dv + upper] = jnp.concatenate(
        [state[0][:upper, :dim], state[0][upper:, :dim]], axis=1
    ).astype(BF16)
    fades = [fade[:, key:], jnp.concatenate([fade[:, :dim], fade[:, :dim]], axis=1)]
    st_ref[dv + upper :] = jnp.concatenate(
        fades + [jnp.zeros((HALO - units, key), F32)], axis=0
    ).astype(BF16)


def kernel(
    n_sp, n_tp,
    wv_ref, wg_ref, wd_ref, qn_ref, kn_ref, gn_ref, qb_ref, kb_ref, gb_ref, v_ref, extra_ref,
    gain_ref, skip_ref, proj_ref, blend_ref, taps_ref,
    mixed_ref,
    wup, wdn, taps, st_own, stbuf, acc_state, out0, meets, heads, piece, up,
    tail, halo, hid, psum, csum, xsum, xbuf, zsum, zbuf, acc_out,
    own_sem, st_send, st_recv, wz_send, wz_recv, wy_send, wy_recv, hx_sems, hc_send,
    hc_recv, tail_send, tail_recv, az_up, az_down, az_recv, ax_send, ax_recv, ac_send, ac_recv, rc_send,
    rc_recv, rx_send, rx_recv, rz_send, rz_recv,
):
    s, t = lax.axis_index("sp"), lax.axis_index("tp")
    nz = n_sp // 2
    z, y = s // 2, s % 2
    zi = z % GROUP
    base = z - zi
    side = s + 1 - 2 * y
    core = t % 2
    tx = lax.rem(t + n_tp // 2, n_tp)
    tc = t + 1 - 2 * core
    tok, cols = skip_ref.shape
    units = v_ref.shape[1]
    kblk, ff = wv_ref.shape
    dblk = wd_ref.shape[1]
    dv = v_ref.shape[2]
    key = qb_ref.shape[1]
    tiles = ff // LANES
    wide_tiles = -(-tiles // GROUP)
    short = wide_tiles * GROUP - tiles
    wide = wide_tiles * LANES
    narrow = wide - LANES

    def rc(src, dst, ss, rs, sp, tp):
        return pltpu.make_async_remote_copy(
            src_ref=src, dst_ref=dst, send_sem=ss, recv_sem=rs,
            device_id=(sp, tp), device_id_type=pl.DeviceIdType.MESH,
        )

    bar = pltpu.get_barrier_semaphore()
    for o in range(1, n_sp):
        pl.semaphore_signal(bar, inc=1, device_id=(lax.rem(s + o, n_sp), t),
                            device_id_type=pl.DeviceIdType.MESH)
    for o in range(1, n_tp):
        pl.semaphore_signal(bar, inc=1, device_id=(s, lax.rem(t + o, n_tp)),
                            device_id_type=pl.DeviceIdType.MESH)
    pl.semaphore_wait(bar, n_sp + n_tp - 2)

    def share(member):
        at = jnp.maximum(member * wide_tiles - core * short, 0)
        thin = jnp.where(core == 0, GROUP - 1, 0)
        return pl.multiple_of(at * LANES, LANES), member == thin

    def each_width(thin, fn):
        if short == 0:
            fn(wide)
            return

        @pl.when(jnp.logical_not(thin))
        def _():
            fn(wide)

        @pl.when(thin)
        def _():
            fn(narrow)

    my_at, my_thin = share(zi)

    def fitting(at, width):
        return pl.multiple_of(jnp.minimum(at, ff - width), LANES)

    def source(m, at, width):
        at = fitting(at, width)
        if m == 2:
            return wd_ref.at[pl.ds(at, width)]
        return (wv_ref, wg_ref)[m].at[:, pl.ds(at, width)]

    def place(m, slot, width):
        if m == 2:
            return wdn.at[slot, pl.ds(0, width)]
        rows = pl.ds(pl.multiple_of(slot * kblk, HALO), kblk)
        return wup.at[rows, pl.ds(m * wide, width)]

    def zcopy(m, o, width):
        zz = lax.rem(z + o, nz)
        at, _ = share(zz % GROUP)
        return rc(source(m, at, width), place(m, s, width), wz_send.at[m, o], wz_recv.at[m, o],
                  zz * 2 + y, t)

    def ycopy(m, o, width):
        slot = lax.rem(z + nz - o, nz) * 2 + y
        first = isinstance(o, int) and o == 0
        src = source(m, my_at, width) if first else place(m, slot, width)
        return rc(src, place(m, slot, width), wy_send.at[m, o], wy_recv.at[m, o], side, t)

    def own(m, width):
        return pltpu.make_async_copy(source(m, my_at, width), place(m, s, width), own_sem.at[m])

    def thin_of(o):
        return share(lax.rem(z + o, nz) % GROUP)[1]

    ranks = ((0, 1, 2, 3), (1, 0, 2, 3), (2, 1, 3, 0), (3, 2, 1, 0))

    def member(o):
        j = jnp.int32(0)
        for r in range(GROUP):
            j = jnp.where(zi == r, ranks[r][o], j)
        return j

    def launch_z(m):
        for o in range(1, nz):
            each_width(thin_of(o), lambda w, o=o: zcopy(m, o, w).start())

    def launch_way(m, upward, where=True):
        for o in range(1, nz):
            way = z + o < nz if upward else z + o >= nz

            @pl.when(jnp.logical_and(way, where))
            def _(o=o):
                each_width(thin_of(o), lambda w: zcopy(m, o, w).start())

    def launch_y(m):
        each_width(my_thin, lambda w: ycopy(m, 0, w).start())

    def relay(m, turns=(1, 2, 3)):
        if nz == GROUP:
            offsets = [lax.rem(zi + GROUP - member(k), GROUP) for k in turns]
        else:
            offsets = range(1, nz) if 1 in turns else ()
        for o in offsets:
            def go(w, o=o):
                zcopy(m, o, w).wait_recv()
                ycopy(m, o, w).start()
            each_width(my_thin, go)

    def settle(m):
        def go(w):
            own(m, w).wait()
            for o in range(nz):
                ycopy(m, o, w).wait_recv()
        each_width(my_thin, go)

    for m in range(3):
        each_width(my_thin, lambda w, m=m: own(m, w).start())
    launch_z(0)
    launch_y(0)
    launch_y(1)
    taps[...] = jnp.zeros_like(taps)

    def load_taps(width):
        for m in range(2):
            for i in range(3):
                taps[m * 3 + i : m * 3 + i + 1, :width] = taps_ref[
                    i, m : m + 1, pl.ds(fitting(my_at, width), width)
                ].astype(F32)
    each_width(my_thin, load_taps)
    if short:
        @pl.when(my_thin)
        def _():
            for m in range(2):
                wup[:, m * wide + narrow : (m + 1) * wide] = jnp.zeros((n_sp * kblk, LANES), BF16)
            for i in range(n_sp):
                wdn[i, narrow:] = jnp.zeros((LANES, dblk), BF16)

    local_attention(
        (qn_ref, qb_ref), (kn_ref, kb_ref), (gn_ref, gb_ref), v_ref, extra_ref, out0, meets, st_own
    )
    st = [None] + [
        rc(st_own, stbuf.at[s], st_send.at[o], st_recv.at[o], lax.rem(s + o, n_sp), t)
        for o in range(1, n_sp)
    ]
    for o in range(1, n_sp):
        @pl.when(s + o < n_sp)
        def _(o=o):
            st[o].start()
    launch_way(1, False)

    acc_state[...] = jnp.zeros_like(acc_state)
    for o in range(n_sp - 1, 0, -1):
        @pl.when(s - o >= 0)
        def _(o=o):
            st[o].wait_recv()
            got = stbuf[s - o].astype(F32)
            fade = dv + dv // 2
            acc_state[:dv] = got[fade : fade + 1] * acc_state[:dv] + got[:dv]
            acc_state[dv:] = got[fade + 1 : fade + 2] * acc_state[dv:] + got[dv:fade]
    for u in range(units):
        at = slice(u * dv, (u + 1) * dv)
        ku = slice(u * key, (u + 1) * key)
        if u:
            total = out0[:, at] + exact(meets[:, ku], acc_state[:dv], NT)
        else:
            dim = qn_ref.shape[0]
            folded = jnp.concatenate([acc_state[dv:, :dim], acc_state[dv:, dim:]], axis=0)
            total = out0[:, at] + exact(meets[:, :dim], folded, NT)
        scale = lax.rsqrt(jnp.mean(total * total, axis=-1, keepdims=True) + EPSILON)
        heads[t, :, at] = (total * scale * gain_ref[0, u : u + 1].astype(F32)).astype(BF16)
    tcx = lax.rem(tc + n_tp // 2, n_tp)
    hx = rc(heads.at[t], heads.at[t], hx_sems.at[0], hx_sems.at[1], s, tx)
    hc = [
        rc(heads.at[slot], heads.at[slot], hc_send.at[i], hc_recv.at[i], s, tc)
        for i, slot in enumerate((t, tx))
    ]
    hx.start()
    hc[0].start()
    relay(0, (1,))
    hx.wait_recv()
    hc[1].start()
    for copy in hc:
        copy.wait_recv()
    whole_heads = jnp.concatenate([heads[i] for i in range(n_tp)], axis=1)
    projected = skip_ref[...].astype(F32) + jnp.dot(
        whole_heads, proj_ref[...], preferred_element_type=F32
    )
    piece[zi, t] = projected.astype(BF16)

    def above(j):
        return rc(piece.at[j, t], piece.at[j, t], az_up.at[j], az_recv.at[j],
                  jnp.where(zi < GROUP - 1, s + 2, s), t)

    def below(j):
        return rc(piece.at[j, t], piece.at[j, t], az_down.at[j], az_recv.at[j],
                  jnp.where(zi > 0, s - 2, s), t)

    def spread(j, up_act, down_act):
        @pl.when(jnp.logical_and(j <= zi, zi < GROUP - 1))
        def _():
            up_act(above(j))

        @pl.when(jnp.logical_and(j >= zi, zi > 0))
        def _():
            down_act(below(j))

    def across(o, tp_slot, ss, rs, to):
        j = member(o)
        return rc(piece.at[j, tp_slot], piece.at[j, tp_slot], ss, rs, s, to)

    ax = [across(o, t, ax_send.at[o], ax_recv.at[o], tx) for o in range(GROUP)]
    ax_got = [across(o, tx, ax_send.at[o], ax_recv.at[o], tx) for o in range(GROUP)]
    ac = [
        [across(o, slot, ac_send.at[o, i], ac_recv.at[o, i], tc) for i, slot in enumerate((t, tx))]
        for o in range(GROUP)
    ]
    ac_got = [
        [across(o, slot, ac_send.at[o, i], ac_recv.at[o, i], tc)
         for i, slot in enumerate((tc, tcx))]
        for o in range(GROUP)
    ]
    def begin(copy):
        copy.start()

    def finish(copy):
        copy.wait_send()

    def collect(o):
        j = member(o)
        above(j).wait_recv()
        spread(j, begin, begin)
        ax[o].start()
        ac[o][0].start()

    ax[0].start()
    spread(zi, begin, begin)
    ac[0][0].start()
    def exchange(o):
        ax_got[o].wait_recv()
        ac[o][1].start()

    @pl.when(zi == 1)
    def _():
        collect(1)

    launch_way(1, True, zi == 1)
    relay(0, (2, 3))
    launch_y(2)

    @pl.when(zi != 1)
    def _():
        collect(1)

    launch_way(1, True, jnp.logical_or(zi == 0, zi == GROUP - 1))
    exchange(0)
    collect(2)
    exchange(1)
    collect(3)
    launch_way(1, True, zi == 2)
    launch_way(2, True)
    launch_way(2, False)
    relay(1, (1, 2, 3))
    exchange(2)
    exchange(3)

    def expand(o):
        j = member(o)
        squares = jnp.zeros((tok, 1), F32)
        for i in range(n_tp):
            part = piece[j, i].astype(F32)
            squares = squares + jnp.sum(part * part, axis=1, keepdims=True)
        scale = lax.rsqrt(squares / (n_tp * cols) + EPSILON)
        total = None
        for i in range(n_tp):
            at = slice(i * cols, (i + 1) * cols)
            normed = (piece[j, i].astype(F32) * scale * blend_ref[:, at]).astype(BF16)
            part = jnp.dot(normed, wup[at], preferred_element_type=F32)
            total = part if total is None else total + part
        rounded = total.astype(BF16)
        tail[o] = rounded[tok - HALO :]
        up[o, HALO:] = rounded.astype(F32)

    def tail_copy(o, slot, to_sp):
        return rc(tail.at[o], halo.at[slot], tail_send.at[o], tail_recv.at[slot], to_sp, t)

    def tail_route(o, act):
        j = member(o)

        @pl.when(y == 0)
        def _():
            act(tail_copy(o, j, side))

        @pl.when(jnp.logical_and(y == 1, j < GROUP - 1))
        def _():
            act(tail_copy(o, jnp.minimum(j + 1, GROUP - 1), side))

        if nz > GROUP:
            @pl.when(jnp.logical_and(jnp.logical_and(y == 1, j == GROUP - 1), z + GROUP < nz))
            def _():
                act(tail_copy(o, 0, jnp.minimum(z + GROUP, nz - 1) * 2))

    def convolve(o):
        j = member(o)
        fresh = jnp.logical_and(jnp.logical_and(y == 0, j == 0), z < GROUP)

        @pl.when(fresh)
        def _():
            up[o, :HALO] = jnp.zeros((HALO, 2 * wide), F32)

        @pl.when(jnp.logical_not(fresh))
        def _():
            tail_copy(o, j, side).wait_recv()
            up[o, :HALO] = halo[j].astype(F32)
        conv = []
        for m in range(2):
            at = slice(m * wide, (m + 1) * wide)
            sums = taps[m * 3 : m * 3 + 1] * up[o, pl.ds(HALO - 2, tok), at]
            sums += taps[m * 3 + 1 : m * 3 + 2] * up[o, pl.ds(HALO - 1, tok), at]
            sums += taps[m * 3 + 2 : m * 3 + 3] * up[o, pl.ds(HALO, tok), at]
            conv.append(sums)
        value, gate = conv
        hid[o] = (gate / (1.0 + jnp.exp(-gate)) * value).astype(BF16)

    settle(0)
    settle(1)
    for o in range(GROUP):
        for copy in ac_got[o]:
            copy.wait_recv()
        expand(o)
        tail_route(o, begin)
        if o:
            relay(2, (o,))
    settle(2)

    per = cols // dblk
    half = n_tp // 2
    order = [3, 2, 1, 0]

    def contract(o):
        for i in range(n_tp):
            for j in range(per):
                psum[o, i, :, j * dblk : (j + 1) * dblk] = jnp.dot(
                    hid[o], wdn[i * per + j], preferred_element_type=F32
                ).astype(BF16)

    rcc = [
        [rc(psum.at[o, i * 2 + 1 - core], csum.at[o, i], rc_send.at[o, i], rc_recv.at[o, i], s, tc)
         for i in range(half)]
        for o in range(GROUP)
    ]
    rx = [rc(xsum.at[o], xbuf.at[o], rx_send.at[o], rx_recv.at[o], s, tx) for o in range(GROUP)]
    def rise(j):
        return rc(zsum.at[j], zbuf.at[0, j], rz_send.at[j], rz_recv.at[0, j],
                  jnp.where(zi < GROUP - 1, s + 2, s), t)

    def fall(j):
        return rc(zsum.at[j], zbuf.at[1, j], rz_send.at[j], rz_recv.at[1, j],
                  jnp.where(zi > 0, s - 2, s), t)

    mine = t // 2
    for step in range(GROUP + 1):
        if step < GROUP:
            o = order[step]
            convolve(o)
            contract(o)
            for copy in rcc[o]:
                copy.start()
        if step:
            o = order[step - 1]
            for copy in rcc[o]:
                copy.wait_recv()
            theirs = half - 1 - mine
            xsum[o] = (psum[o, theirs * 2 + core].astype(F32) + csum[o, theirs].astype(F32)).astype(
                BF16
            )
            rx[o].start()
    def reduced(o):
        return psum[o, t].astype(F32) + csum[o, mine].astype(F32) + xbuf[o].astype(F32)

    for o in order[:-1]:
        j = member(o)
        rx[o].wait_recv()

        @pl.when(j > zi)
        def _(o=o, j=j):
            @pl.when(zi > 0)
            def _():
                rise(j).wait_recv()
                zsum[j] = (reduced(o) + zbuf[0, j].astype(F32)).astype(BF16)

            @pl.when(zi == 0)
            def _():
                zsum[j] = reduced(o).astype(BF16)
            rise(j).start()

        @pl.when(j < zi)
        def _(o=o, j=j):
            @pl.when(zi < GROUP - 1)
            def _():
                fall(j).wait_recv()
                zsum[j] = (reduced(o) + zbuf[1, j].astype(F32)).astype(BF16)

            @pl.when(zi == GROUP - 1)
            def _():
                zsum[j] = reduced(o).astype(BF16)
            fall(j).start()
    rx[0].wait_recv()
    acc_out[...] = reduced(0) + piece[zi, t].astype(F32)

    @pl.when(zi > 0)
    def _():
        rise(zi).wait_recv()
        acc_out[...] += zbuf[0, zi].astype(F32)

    @pl.when(zi < GROUP - 1)
    def _():
        fall(zi).wait_recv()
        acc_out[...] += zbuf[1, zi].astype(F32)
    mixed_ref[...] = acc_out[...].astype(BF16)

    for o in range(1, n_sp):
        @pl.when(s + o < n_sp)
        def _(o=o):
            st[o].wait_send()

    for m in range(3):
        for o in range(1, nz):
            each_width(thin_of(o), lambda w, m=m, o=o: zcopy(m, o, w).wait_send())

        def drain(w, m=m):
            for o in range(nz):
                ycopy(m, o, w).wait_send()
        each_width(my_thin, drain)
    for o in range(GROUP):
        tail_route(o, finish)
        spread(member(o), finish, finish)
    for o in order[:-1]:
        rise(member(o)).wait_send()
    for copy in [hx] + hc + ax + rx:
        copy.wait_send()
    for o in range(GROUP):
        for copy in ac[o] + rcc[o]:
            copy.wait_send()


def local(
    n_sp, n_tp,
    skip_stream,
    narrow_lookup_matrix,
    narrow_probe_matrix,
    narrow_retention_logits,
    broad_lookup_matrix,
    broad_probe_matrix,
    broad_retention_logits,
    content_vectors,
    extra_log_retention,
    per_branch_scaling,
    final_projection_matrix,
    channel_blend_scaling,
    switch_expansion_matrix,
    content_expansion_matrix,
    convolution_kernel,
    contraction_matrix,
):
    tok, cols = skip_stream.shape
    heads = content_vectors.shape[1]
    dv = content_vectors.shape[3]
    narrow = narrow_lookup_matrix.shape[1]
    broad = broad_lookup_matrix.shape[1]
    units = 2 * heads
    kblk, ff = content_expansion_matrix.shape
    dblk = contraction_matrix.shape[1]
    assert heads == 1 and n_tp == 4 and 2 * narrow == broad
    values = content_vectors.reshape(tok, units, dv)
    extra = extra_log_retention.transpose(1, 2, 0)
    blend = channel_blend_scaling.astype(F32).reshape(1, -1)
    wide = -(-(ff // LANES) // GROUP) * LANES
    nz = n_sp // 2
    width = units * broad
    model = n_tp * cols
    dma = pltpu.SemaphoreType.DMA
    vmem = pl.BlockSpec(memory_space=pltpu.VMEM)
    anywhere = pl.BlockSpec(memory_space=pltpu.HBM)
    return pl.pallas_call(
        functools.partial(kernel, n_sp, n_tp),
        out_shape=jax.ShapeDtypeStruct((tok, cols), BF16),
        in_specs=[anywhere] * 3 + [vmem] * 13,
        out_specs=vmem,
        scratch_shapes=[
            pltpu.VMEM((model, 2 * wide), BF16),
            pltpu.VMEM((n_sp, wide, dblk), BF16),
            pltpu.VMEM((8, wide), F32),
            pltpu.VMEM((dv + dv // 2 + HALO, broad), BF16),
            pltpu.VMEM((n_sp, dv + dv // 2 + HALO, broad), BF16),
            pltpu.VMEM((dv + dv // 2, broad), F32),
            pltpu.VMEM((tok, units * dv), F32),
            pltpu.VMEM((tok, width), F32),
            pltpu.VMEM((n_tp, tok, units * dv), BF16),
            pltpu.VMEM((GROUP, n_tp, tok, cols), BF16),
            pltpu.VMEM((GROUP, HALO + tok, 2 * wide), F32),
            pltpu.VMEM((GROUP, HALO, 2 * wide), BF16),
            pltpu.VMEM((GROUP, HALO, 2 * wide), BF16),
            pltpu.VMEM((GROUP, tok, wide), BF16),
            pltpu.VMEM((GROUP, n_tp, tok, cols), BF16),
            pltpu.VMEM((GROUP, n_tp // 2, tok, cols), BF16),
            pltpu.VMEM((GROUP, tok, cols), BF16),
            pltpu.VMEM((GROUP, tok, cols), BF16),
            pltpu.VMEM((GROUP, tok, cols), BF16),
            pltpu.VMEM((2, GROUP, tok, cols), BF16),
            pltpu.VMEM((tok, cols), F32),
            dma((3,)),
            dma((n_sp,)), dma((n_sp,)),
            dma((3, nz)), dma((3, nz)), dma((3, nz)), dma((3, nz)),
            dma((2,)), dma((2,)), dma((2,)), dma((GROUP,)), dma((GROUP,)),
            dma((GROUP,)), dma((GROUP,)), dma((GROUP,)), dma((GROUP,)), dma((GROUP,)),
            dma((GROUP, 2)), dma((GROUP, 2)), dma((GROUP, 2)), dma((GROUP, 2)),
            dma((GROUP,)), dma((GROUP,)), dma((GROUP,)), dma((2, GROUP)),
        ],
        compiler_params=pltpu.CompilerParams(
            collective_id=0, has_side_effects=True, vmem_limit_bytes=58 * 1024 * 1024
        ),
    )(
        content_expansion_matrix, switch_expansion_matrix, contraction_matrix, narrow_lookup_matrix.T,
        narrow_probe_matrix.T, narrow_retention_logits.T, broad_lookup_matrix, broad_probe_matrix,
        broad_retention_logits, values, extra, per_branch_scaling, skip_stream,
        final_projection_matrix, blend, convolution_kernel,
    )


def solution(mesh):
    in_specs = (
        P("sp", "tp"),
        P("sp", "tp"),
        P("sp", "tp"),
        P("sp", "tp"),
        P("sp", "tp"),
        P("sp", "tp"),
        P("sp", "tp"),
        P("sp", "tp", None, None),
        P("sp", None, "tp"),
        P("tp", None, None),
        P(None, "tp"),
        P(),
        P("sp", "tp"),
        P("sp", "tp"),
        P(None, None, "tp"),
        P("tp", "sp"),
    )
    out_specs = P("sp", "tp")
    body = functools.partial(local, mesh.shape["sp"], mesh.shape["tp"])
    return jax.shard_map(body, mesh=mesh, in_specs=in_specs, out_specs=out_specs, check_vma=False)
```

```python
import functools

import jax
import jax.numpy as jnp
from jax import lax
from jax.experimental import pallas as pl
from jax.experimental.pallas import tpu as pltpu
from jax.sharding import PartitionSpec as P

BLOCK = 64
HALO = 16
LANES = 128
GROUP = 4
EPSILON = 1e-06
SOFTENING = 16.0
HIGHEST = lax.Precision.HIGHEST
F32 = jnp.float32
BF16 = jnp.bfloat16
NT = (((1,), (1,)), ((), ()))
TN = (((0,), (0,)), ((), ()))


def exact(a, b, dims):
    return lax.dot_general(a, b, dims, precision=HIGHEST, preferred_element_type=F32)


def local_attention(
    q_refs, k_refs, g_refs, v_ref, extra_ref, out_ref, meets_ref, st_ref
):
    tok, units, dv = v_ref.shape
    key = q_refs[1].shape[1]
    dim = q_refs[0].shape[0]

    def join(refs, scale):
        first = jnp.transpose(refs[0][...].astype(F32))
        second = refs[1][...].astype(F32)
        if scale:
            first = first * dim ** (-0.5)
            second = second * key ** (-0.5)
        if dim < key:
            first = jnp.concatenate([first, jnp.zeros((tok, key - dim), F32)], axis=1)
        return jnp.concatenate([first, second], axis=1)

    gate = join(g_refs, False)
    query_all = join(q_refs, True)
    keys_all = join(k_refs, False)
    soft = jnp.minimum(gate, 0.0) - jnp.log1p(jnp.exp(-jnp.abs(gate)))
    extra = jnp.transpose(
        jnp.concatenate([extra_ref[u] for u in range(units)] + [jnp.zeros((8 - units, tok), F32)], axis=0)
    )
    decay = jnp.concatenate(
        [
            soft[:, u * key : (u + 1) * key] * (1.0 / SOFTENING) + extra[:, u : u + 1]
            for u in range(units)
        ],
        axis=1,
    )
    values_all = v_ref[...].astype(F32)
    row = lax.broadcasted_iota(jnp.int32, (BLOCK, BLOCK), 0)
    col = lax.broadcasted_iota(jnp.int32, (BLOCK, BLOCK), 1)
    lower = row >= col
    tri = jnp.where(lower, 1.0, 0.0)
    plain = (((1,), (0,)), ((), ()))
    before = jnp.zeros((1, units * key), F32)
    state = [jnp.zeros((dv, key), F32) for _ in range(units)]
    for n in range(tok // BLOCK):
        rows = slice(n * BLOCK, (n + 1) * BLOCK)
        inner = exact(tri, decay[rows], plain)
        last = inner[BLOCK - 1 : BLOCK]
        middle = inner[BLOCK // 2 - 1 : BLOCK // 2]
        query = query_all[rows]
        keys = keys_all[rows]
        query_mid = query * jnp.exp(inner - middle)
        key_mid = keys * jnp.exp(middle - inner)
        query_carry = query * jnp.exp(inner)
        key_carry = keys * jnp.exp(last - inner)
        meets_ref[rows] = query_carry * jnp.exp(before)
        gone = jnp.exp(last)
        for u in range(units):
            at = slice(u * key, (u + 1) * key)
            vu = values_all[rows, u, :]
            scores = exact(query_mid[:, at], key_mid[:, at], NT)
            out = exact(jnp.where(lower, scores, 0.0), vu, plain)
            if n:
                out = out + exact(query_carry[:, at], state[u], NT)
            out_ref[rows, u * dv : (u + 1) * dv] = out
            state[u] = gone[:, at] * state[u] + exact(vu, key_carry[:, at], TN)
        before = before + last
    fade = jnp.exp(before)
    upper = dv // 2
    st_ref[:dv] = state[1].astype(BF16)
    st_ref[dv : dv + upper] = jnp.concatenate(
        [state[0][:upper, :dim], state[0][upper:, :dim]], axis=1
    ).astype(BF16)
    fades = [fade[:, key:], jnp.concatenate([fade[:, :dim], fade[:, :dim]], axis=1)]
    st_ref[dv + upper :] = jnp.concatenate(
        fades + [jnp.zeros((HALO - units, key), F32)], axis=0
    ).astype(BF16)


def kernel(
    n_sp, n_tp,
    wv_ref, wg_ref, wd_ref, qn_ref, kn_ref, gn_ref, qb_ref, kb_ref, gb_ref, v_ref, extra_ref,
    gain_ref, skip_ref, proj_ref, blend_ref, taps_ref,
    mixed_ref,
    wup, wdn, taps, st_own, stbuf, acc_state, out0, meets, heads, piece, up,
    tail, halo, hid, psum, csum, xsum, xbuf, zsum, zbuf, acc_out,
    own_sem, st_send, st_recv, wz_send, wz_recv, wy_send, wy_recv, hx_sems, hc_send,
    hc_recv, tail_send, tail_recv, az_up, az_down, az_recv, ax_send, ax_recv, ac_send, ac_recv, rc_send,
    rc_recv, rx_send, rx_recv, rz_send, rz_recv,
):
    s, t = lax.axis_index("sp"), lax.axis_index("tp")
    nz = n_sp // 2
    z, y = s // 2, s % 2
    zi = z % GROUP
    base = z - zi
    side = s + 1 - 2 * y
    core = t % 2
    tx = lax.rem(t + n_tp // 2, n_tp)
    tc = t + 1 - 2 * core
    tok, cols = skip_ref.shape
    units = v_ref.shape[1]
    kblk, ff = wv_ref.shape
    dblk = wd_ref.shape[1]
    dv = v_ref.shape[2]
    key = qb_ref.shape[1]
    tiles = ff // LANES
    wide_tiles = -(-tiles // GROUP)
    short = wide_tiles * GROUP - tiles
    wide = wide_tiles * LANES
    narrow = wide - LANES

    def rc(src, dst, ss, rs, sp, tp):
        return pltpu.make_async_remote_copy(
            src_ref=src, dst_ref=dst, send_sem=ss, recv_sem=rs,
            device_id=(sp, tp), device_id_type=pl.DeviceIdType.MESH,
        )

    bar = pltpu.get_barrier_semaphore()
    for o in range(1, n_sp):
        pl.semaphore_signal(bar, inc=1, device_id=(lax.rem(s + o, n_sp), t),
                            device_id_type=pl.DeviceIdType.MESH)
    for o in range(1, n_tp):
        pl.semaphore_signal(bar, inc=1, device_id=(s, lax.rem(t + o, n_tp)),
                            device_id_type=pl.DeviceIdType.MESH)
    pl.semaphore_wait(bar, n_sp + n_tp - 2)

    def share(member):
        at = jnp.maximum(member * wide_tiles - core * short, 0)
        thin = jnp.where(core == 0, GROUP - 1, 0)
        return pl.multiple_of(at * LANES, LANES), member == thin

    def each_width(thin, fn):
        if short == 0:
            fn(wide)
            return

        @pl.when(jnp.logical_not(thin))
        def _():
            fn(wide)

        @pl.when(thin)
        def _():
            fn(narrow)

    my_at, my_thin = share(zi)

    def fitting(at, width):
        return pl.multiple_of(jnp.minimum(at, ff - width), LANES)

    def source(m, at, width):
        at = fitting(at, width)
        if m == 2:
            return wd_ref.at[pl.ds(at, width)]
        return (wv_ref, wg_ref)[m].at[:, pl.ds(at, width)]

    def place(m, slot, width):
        if m == 2:
            return wdn.at[slot, pl.ds(0, width)]
        rows = pl.ds(pl.multiple_of(slot * kblk, HALO), kblk)
        return wup.at[rows, pl.ds(m * wide, width)]

    def zcopy(m, o, width):
        zz = lax.rem(z + o, nz)
        at, _ = share(zz % GROUP)
        return rc(source(m, at, width), place(m, s, width), wz_send.at[m, o], wz_recv.at[m, o],
                  zz * 2 + y, t)

    def ycopy(m, o, width):
        slot = lax.rem(z + nz - o, nz) * 2 + y
        first = isinstance(o, int) and o == 0
        src = source(m, my_at, width) if first else place(m, slot, width)
        return rc(src, place(m, slot, width), wy_send.at[m, o], wy_recv.at[m, o], side, t)

    def own(m, width):
        return pltpu.make_async_copy(source(m, my_at, width), place(m, s, width), own_sem.at[m])

    def thin_of(o):
        return share(lax.rem(z + o, nz) % GROUP)[1]

    ranks = ((0, 1, 2, 3), (1, 0, 2, 3), (2, 1, 3, 0), (3, 2, 1, 0))

    def member(o):
        j = jnp.int32(0)
        for r in range(GROUP):
            j = jnp.where(zi == r, ranks[r][o], j)
        return j

    def launch_z(m):
        for o in range(1, nz):
            each_width(thin_of(o), lambda w, o=o: zcopy(m, o, w).start())

    def launch_way(m, upward, where=True):
        for o in range(1, nz):
            way = z + o < nz if upward else z + o >= nz

            @pl.when(jnp.logical_and(way, where))
            def _(o=o):
                each_width(thin_of(o), lambda w: zcopy(m, o, w).start())

    def launch_y(m):
        each_width(my_thin, lambda w: ycopy(m, 0, w).start())

    def relay(m, turns=(1, 2, 3)):
        if nz == GROUP:
            offsets = [lax.rem(zi + GROUP - member(k), GROUP) for k in turns]
        else:
            offsets = range(1, nz) if 1 in turns else ()
        for o in offsets:
            def go(w, o=o):
                zcopy(m, o, w).wait_recv()
                ycopy(m, o, w).start()
            each_width(my_thin, go)

    def settle(m):
        def go(w):
            own(m, w).wait()
            for o in range(nz):
                ycopy(m, o, w).wait_recv()
        each_width(my_thin, go)

    for m in range(3):
        each_width(my_thin, lambda w, m=m: own(m, w).start())
    launch_z(0)
    launch_y(0)
    launch_y(1)
    taps[...] = jnp.zeros_like(taps)

    def load_taps(width):
        for m in range(2):
            for i in range(3):
                taps[m * 3 + i : m * 3 + i + 1, :width] = taps_ref[
                    i, m : m + 1, pl.ds(fitting(my_at, width), width)
                ].astype(F32)
    each_width(my_thin, load_taps)
    if short:
        @pl.when(my_thin)
        def _():
            for m in range(2):
                wup[:, m * wide + narrow : (m + 1) * wide] = jnp.zeros((n_sp * kblk, LANES), BF16)
            for i in range(n_sp):
                wdn[i, narrow:] = jnp.zeros((LANES, dblk), BF16)

    local_attention(
        (qn_ref, qb_ref), (kn_ref, kb_ref), (gn_ref, gb_ref), v_ref, extra_ref, out0, meets, st_own
    )
    st = [None] + [
        rc(st_own, stbuf.at[s], st_send.at[o], st_recv.at[o], lax.rem(s + o, n_sp), t)
        for o in range(1, n_sp)
    ]
    for o in range(1, n_sp):
        @pl.when(s + o < n_sp)
        def _(o=o):
            st[o].start()
    launch_way(1, False)

    acc_state[...] = jnp.zeros_like(acc_state)
    for o in range(n_sp - 1, 0, -1):
        @pl.when(s - o >= 0)
        def _(o=o):
            st[o].wait_recv()
            got = stbuf[s - o].astype(F32)
            fade = dv + dv // 2
            acc_state[:dv] = got[fade : fade + 1] * acc_state[:dv] + got[:dv]
            acc_state[dv:] = got[fade + 1 : fade + 2] * acc_state[dv:] + got[dv:fade]
    for u in range(units):
        at = slice(u * dv, (u + 1) * dv)
        ku = slice(u * key, (u + 1) * key)
        if u:
            total = out0[:, at] + exact(meets[:, ku], acc_state[:dv], NT)
        else:
            dim = qn_ref.shape[0]
            folded = jnp.concatenate([acc_state[dv:, :dim], acc_state[dv:, dim:]], axis=0)
            total = out0[:, at] + exact(meets[:, :dim], folded, NT)
        scale = lax.rsqrt(jnp.mean(total * total, axis=-1, keepdims=True) + EPSILON)
        heads[t, :, at] = (total * scale * gain_ref[0, u : u + 1].astype(F32)).astype(BF16)
    tcx = lax.rem(tc + n_tp // 2, n_tp)
    hx = rc(heads.at[t], heads.at[t], hx_sems.at[0], hx_sems.at[1], s, tx)
    hc = [
        rc(heads.at[slot], heads.at[slot], hc_send.at[i], hc_recv.at[i], s, tc)
        for i, slot in enumerate((t, tx))
    ]
    hx.start()
    hc[0].start()
    relay(0, (1,))
    hx.wait_recv()
    hc[1].start()
    for copy in hc:
        copy.wait_recv()
    whole_heads = jnp.concatenate([heads[i] for i in range(n_tp)], axis=1)
    projected = skip_ref[...].astype(F32) + jnp.dot(
        whole_heads, proj_ref[...], preferred_element_type=F32
    )
    piece[zi, t] = projected.astype(BF16)

    def above(j):
        return rc(piece.at[j, t], piece.at[j, t], az_up.at[j], az_recv.at[j],
                  jnp.where(zi < GROUP - 1, s + 2, s), t)

    def below(j):
        return rc(piece.at[j, t], piece.at[j, t], az_down.at[j], az_recv.at[j],
                  jnp.where(zi > 0, s - 2, s), t)

    def spread(j, up_act, down_act):
        @pl.when(jnp.logical_and(j <= zi, zi < GROUP - 1))
        def _():
            up_act(above(j))

        @pl.when(jnp.logical_and(j >= zi, zi > 0))
        def _():
            down_act(below(j))

    def across(o, tp_slot, ss, rs, to):
        j = member(o)
        return rc(piece.at[j, tp_slot], piece.at[j, tp_slot], ss, rs, s, to)

    ax = [across(o, t, ax_send.at[o], ax_recv.at[o], tx) for o in range(GROUP)]
    ax_got = [across(o, tx, ax_send.at[o], ax_recv.at[o], tx) for o in range(GROUP)]
    ac = [
        [across(o, slot, ac_send.at[o, i], ac_recv.at[o, i], tc) for i, slot in enumerate((t, tx))]
        for o in range(GROUP)
    ]
    ac_got = [
        [across(o, slot, ac_send.at[o, i], ac_recv.at[o, i], tc)
         for i, slot in enumerate((tc, tcx))]
        for o in range(GROUP)
    ]
    def begin(copy):
        copy.start()

    def finish(copy):
        copy.wait_send()

    def collect(o):
        j = member(o)
        above(j).wait_recv()
        spread(j, begin, begin)
        ax[o].start()
        ac[o][0].start()

    ax[0].start()
    spread(zi, begin, begin)
    ac[0][0].start()
    def exchange(o):
        ax_got[o].wait_recv()
        ac[o][1].start()

    @pl.when(zi == 1)
    def _():
        collect(1)

    launch_way(1, True, zi == 1)
    relay(0, (2, 3))
    launch_y(2)

    @pl.when(zi != 1)
    def _():
        collect(1)

    launch_way(1, True, jnp.logical_or(zi == 0, zi == GROUP - 1))
    launch_way(2, True, zi == 0)
    launch_way(1, True, zi == 2)
    exchange(0)

    @pl.when(zi == 0)
    def _():
        relay(1, (1,))

    @pl.when(jnp.logical_or(zi == 1, zi == 2))
    def _():
        relay(1, (2,))

    collect(2)
    exchange(1)

    @pl.when(zi == 0)
    def _():
        relay(1, (2,))

    @pl.when(zi == 1)
    def _():
        relay(1, (3,))

    @pl.when(zi == GROUP - 1)
    def _():
        relay(1, (1,))

    collect(3)
    launch_way(2, True, zi > 0)
    launch_way(2, False)
    for r, turns in enumerate(((3,), (1,), (1, 3), (2, 3))):
        @pl.when(zi == r)
        def _(turns=turns):
            relay(1, turns)

    exchange(2)
    exchange(3)

    def expand(o):
        j = member(o)
        squares = jnp.zeros((tok, 1), F32)
        for i in range(n_tp):
            part = piece[j, i].astype(F32)
            squares = squares + jnp.sum(part * part, axis=1, keepdims=True)
        scale = lax.rsqrt(squares / (n_tp * cols) + EPSILON)
        total = None
        for i in range(n_tp):
            at = slice(i * cols, (i + 1) * cols)
            normed = (piece[j, i].astype(F32) * scale * blend_ref[:, at]).astype(BF16)
            part = jnp.dot(normed, wup[at], preferred_element_type=F32)
            total = part if total is None else total + part
        rounded = total.astype(BF16)
        tail[o] = rounded[tok - HALO :]
        up[o, HALO:] = rounded.astype(F32)

    def tail_copy(o, slot, to_sp):
        return rc(tail.at[o], halo.at[slot], tail_send.at[o], tail_recv.at[slot], to_sp, t)

    def tail_route(o, act):
        j = member(o)

        @pl.when(y == 0)
        def _():
            act(tail_copy(o, j, side))

        @pl.when(jnp.logical_and(y == 1, j < GROUP - 1))
        def _():
            act(tail_copy(o, jnp.minimum(j + 1, GROUP - 1), side))

        if nz > GROUP:
            @pl.when(jnp.logical_and(jnp.logical_and(y == 1, j == GROUP - 1), z + GROUP < nz))
            def _():
                act(tail_copy(o, 0, jnp.minimum(z + GROUP, nz - 1) * 2))

    def convolve(o):
        j = member(o)
        fresh = jnp.logical_and(jnp.logical_and(y == 0, j == 0), z < GROUP)

        @pl.when(fresh)
        def _():
            up[o, :HALO] = jnp.zeros((HALO, 2 * wide), F32)

        @pl.when(jnp.logical_not(fresh))
        def _():
            tail_copy(o, j, side).wait_recv()
            up[o, :HALO] = halo[j].astype(F32)
        conv = []
        for m in range(2):
            at = slice(m * wide, (m + 1) * wide)
            sums = taps[m * 3 : m * 3 + 1] * up[o, pl.ds(HALO - 2, tok), at]
            sums += taps[m * 3 + 1 : m * 3 + 2] * up[o, pl.ds(HALO - 1, tok), at]
            sums += taps[m * 3 + 2 : m * 3 + 3] * up[o, pl.ds(HALO, tok), at]
            conv.append(sums)
        value, gate = conv
        hid[o] = (gate / (1.0 + jnp.exp(-gate)) * value).astype(BF16)

    settle(0)
    settle(1)
    def relay_down(plan):
        for r, turns in plan.items():
            @pl.when(zi == r)
            def _(turns=turns):
                relay(2, turns)

    down_plan = (
        {0: (3,), 3: (2,)}, {1: (1,), 2: (1,), 3: (3,)}, {1: (2,), 2: (2,)}, {1: (3,), 2: (3,)}
    )
    relay_down({0: (1, 2), 3: (1,)})
    for o in range(GROUP):
        for copy in ac_got[o]:
            copy.wait_recv()
        expand(o)
        tail_route(o, begin)
        relay_down(down_plan[o])
    settle(2)

    per = cols // dblk
    half = n_tp // 2
    order = [3, 2, 1, 0]

    def contract(o):
        for i in range(n_tp):
            for j in range(per):
                psum[o, i, :, j * dblk : (j + 1) * dblk] = jnp.dot(
                    hid[o], wdn[i * per + j], preferred_element_type=F32
                ).astype(BF16)

    rcc = [
        [rc(psum.at[o, i * 2 + 1 - core], csum.at[o, i], rc_send.at[o, i], rc_recv.at[o, i], s, tc)
         for i in range(half)]
        for o in range(GROUP)
    ]
    rx = [rc(xsum.at[o], xbuf.at[o], rx_send.at[o], rx_recv.at[o], s, tx) for o in range(GROUP)]
    def rise(j):
        return rc(zsum.at[j], zbuf.at[0, j], rz_send.at[j], rz_recv.at[0, j],
                  jnp.where(zi < GROUP - 1, s + 2, s), t)

    def fall(j):
        return rc(zsum.at[j], zbuf.at[1, j], rz_send.at[j], rz_recv.at[1, j],
                  jnp.where(zi > 0, s - 2, s), t)

    mine = t // 2
    for step in range(GROUP + 1):
        if step < GROUP:
            o = order[step]
            convolve(o)
            contract(o)
            for copy in rcc[o]:
                copy.start()
        if step:
            o = order[step - 1]
            for copy in rcc[o]:
                copy.wait_recv()
            theirs = half - 1 - mine
            xsum[o] = (psum[o, theirs * 2 + core].astype(F32) + csum[o, theirs].astype(F32)).astype(
                BF16
            )
            rx[o].start()
    def reduced(o):
        return psum[o, t].astype(F32) + csum[o, mine].astype(F32) + xbuf[o].astype(F32)

    for o in order[:-1]:
        j = member(o)
        rx[o].wait_recv()

        @pl.when(j > zi)
        def _(o=o, j=j):
            @pl.when(zi > 0)
            def _():
                rise(j).wait_recv()
                zsum[j] = (reduced(o) + zbuf[0, j].astype(F32)).astype(BF16)

            @pl.when(zi == 0)
            def _():
                zsum[j] = reduced(o).astype(BF16)
            rise(j).start()

        @pl.when(j < zi)
        def _(o=o, j=j):
            @pl.when(zi < GROUP - 1)
            def _():
                fall(j).wait_recv()
                zsum[j] = (reduced(o) + zbuf[1, j].astype(F32)).astype(BF16)

            @pl.when(zi == GROUP - 1)
            def _():
                zsum[j] = reduced(o).astype(BF16)
            fall(j).start()
    rx[0].wait_recv()
    acc_out[...] = reduced(0) + piece[zi, t].astype(F32)

    @pl.when(zi > 0)
    def _():
        rise(zi).wait_recv()
        acc_out[...] += zbuf[0, zi].astype(F32)

    @pl.when(zi < GROUP - 1)
    def _():
        fall(zi).wait_recv()
        acc_out[...] += zbuf[1, zi].astype(F32)
    mixed_ref[...] = acc_out[...].astype(BF16)

    for o in range(1, n_sp):
        @pl.when(s + o < n_sp)
        def _(o=o):
            st[o].wait_send()

    for m in range(3):
        for o in range(1, nz):
            each_width(thin_of(o), lambda w, m=m, o=o: zcopy(m, o, w).wait_send())

        def drain(w, m=m):
            for o in range(nz):
                ycopy(m, o, w).wait_send()
        each_width(my_thin, drain)
    for o in range(GROUP):
        tail_route(o, finish)
        spread(member(o), finish, finish)
    for o in order[:-1]:
        rise(member(o)).wait_send()
    for copy in [hx] + hc + ax + rx:
        copy.wait_send()
    for o in range(GROUP):
        for copy in ac[o] + rcc[o]:
            copy.wait_send()


def local(
    n_sp, n_tp,
    skip_stream,
    narrow_lookup_matrix,
    narrow_probe_matrix,
    narrow_retention_logits,
    broad_lookup_matrix,
    broad_probe_matrix,
    broad_retention_logits,
    content_vectors,
    extra_log_retention,
    per_branch_scaling,
    final_projection_matrix,
    channel_blend_scaling,
    switch_expansion_matrix,
    content_expansion_matrix,
    convolution_kernel,
    contraction_matrix,
):
    tok, cols = skip_stream.shape
    heads = content_vectors.shape[1]
    dv = content_vectors.shape[3]
    narrow = narrow_lookup_matrix.shape[1]
    broad = broad_lookup_matrix.shape[1]
    units = 2 * heads
    kblk, ff = content_expansion_matrix.shape
    dblk = contraction_matrix.shape[1]
    assert heads == 1 and n_tp == 4 and 2 * narrow == broad
    values = content_vectors.reshape(tok, units, dv)
    extra = extra_log_retention.transpose(1, 2, 0)
    blend = channel_blend_scaling.astype(F32).reshape(1, -1)
    wide = -(-(ff // LANES) // GROUP) * LANES
    nz = n_sp // 2
    width = units * broad
    model = n_tp * cols
    dma = pltpu.SemaphoreType.DMA
    vmem = pl.BlockSpec(memory_space=pltpu.VMEM)
    anywhere = pl.BlockSpec(memory_space=pltpu.HBM)
    return pl.pallas_call(
        functools.partial(kernel, n_sp, n_tp),
        out_shape=jax.ShapeDtypeStruct((tok, cols), BF16),
        in_specs=[anywhere] * 3 + [vmem] * 13,
        out_specs=vmem,
        scratch_shapes=[
            pltpu.VMEM((model, 2 * wide), BF16),
            pltpu.VMEM((n_sp, wide, dblk), BF16),
            pltpu.VMEM((8, wide), F32),
            pltpu.VMEM((dv + dv // 2 + HALO, broad), BF16),
            pltpu.VMEM((n_sp, dv + dv // 2 + HALO, broad), BF16),
            pltpu.VMEM((dv + dv // 2, broad), F32),
            pltpu.VMEM((tok, units * dv), F32),
            pltpu.VMEM((tok, width), F32),
            pltpu.VMEM((n_tp, tok, units * dv), BF16),
            pltpu.VMEM((GROUP, n_tp, tok, cols), BF16),
            pltpu.VMEM((GROUP, HALO + tok, 2 * wide), F32),
            pltpu.VMEM((GROUP, HALO, 2 * wide), BF16),
            pltpu.VMEM((GROUP, HALO, 2 * wide), BF16),
            pltpu.VMEM((GROUP, tok, wide), BF16),
            pltpu.VMEM((GROUP, n_tp, tok, cols), BF16),
            pltpu.VMEM((GROUP, n_tp // 2, tok, cols), BF16),
            pltpu.VMEM((GROUP, tok, cols), BF16),
            pltpu.VMEM((GROUP, tok, cols), BF16),
            pltpu.VMEM((GROUP, tok, cols), BF16),
            pltpu.VMEM((2, GROUP, tok, cols), BF16),
            pltpu.VMEM((tok, cols), F32),
            dma((3,)),
            dma((n_sp,)), dma((n_sp,)),
            dma((3, nz)), dma((3, nz)), dma((3, nz)), dma((3, nz)),
            dma((2,)), dma((2,)), dma((2,)), dma((GROUP,)), dma((GROUP,)),
            dma((GROUP,)), dma((GROUP,)), dma((GROUP,)), dma((GROUP,)), dma((GROUP,)),
            dma((GROUP, 2)), dma((GROUP, 2)), dma((GROUP, 2)), dma((GROUP, 2)),
            dma((GROUP,)), dma((GROUP,)), dma((GROUP,)), dma((2, GROUP)),
        ],
        compiler_params=pltpu.CompilerParams(
            collective_id=0, has_side_effects=True, vmem_limit_bytes=58 * 1024 * 1024
        ),
    )(
        content_expansion_matrix, switch_expansion_matrix, contraction_matrix, narrow_lookup_matrix.T,
        narrow_probe_matrix.T, narrow_retention_logits.T, broad_lookup_matrix, broad_probe_matrix,
        broad_retention_logits, values, extra, per_branch_scaling, skip_stream,
        final_projection_matrix, blend, convolution_kernel,
    )


def solution(mesh):
    in_specs = (
        P("sp", "tp"),
        P("sp", "tp"),
        P("sp", "tp"),
        P("sp", "tp"),
        P("sp", "tp"),
        P("sp", "tp"),
        P("sp", "tp"),
        P("sp", "tp", None, None),
        P("sp", None, "tp"),
        P("tp", None, None),
        P(None, "tp"),
        P(),
        P("sp", "tp"),
        P("sp", "tp"),
        P(None, None, "tp"),
        P("tp", "sp"),
    )
    out_specs = P("sp", "tp")
    body = functools.partial(local, mesh.shape["sp"], mesh.shape["tp"])
    return jax.shard_map(body, mesh=mesh, in_specs=in_specs, out_specs=out_specs, check_vma=False)
```
